32 devices in a mesh: grp: 2 (over y), tp: 4 (over z), dp: 4 (over x, core).
Axes of the slice: x: 2, y: 2, z: 4, core: 2. Of those that a mesh axis runs over, the one named last changes fastest.
Arguments:
- tokens: bfloat16 [128, 4096], P('grp', 'dp'), parts along dimension 0, may hold values from -50 to 50
- lengths: int32 [128], P(('grp', 'dp')), parts along dimension 0, may hold values from 1 to 24, as said below
- norm_gain: float32 [2, 4096], P(None, 'dp'), may hold values from 0.1 to 1.9
- w_z: bfloat16 [2, 4096, 4096], P(None, 'dp', 'tp'), may hold values from -0.09375 to 0.09375
- w_x: bfloat16 [2, 4096, 4096], P(None, 'dp', 'tp'), may hold values from -0.09375 to 0.09375
- w_b: bfloat16 [2, 4096, 2048], P(None, 'dp', 'tp'), may hold values from -0.09375 to 0.09375
- w_c: bfloat16 [2, 4096, 2048], P(None, 'dp', 'tp'), may hold values from -0.09375 to 0.09375
- w_dt: bfloat16 [2, 4096, 64], P(None, 'dp'), may hold values from -0.09375 to 0.09375
- conv_weight: bfloat16 [2, 4, 8192], P(None, None, 'tp'), may hold values from -3 to 3
- dt_bias: float32 [2, 64], P(None, 'tp'), may hold values from -6 to -1.5
- a_log: float32 [2, 64], P(None, 'tp'), may hold values from 0 to 2.77
- d_skip: float32 [2, 64], P(None, 'tp'), may hold values from 0.1 to 1.9
- out_gain: float32 [2, 4096], P(None, 'tp'), may hold values from 0.1 to 1.9
- w_out: bfloat16 [2, 4096, 4096], P(None, 'tp', 'dp'), may hold values from -0.09375 to 0.09375
- conv_state: bfloat16 [2, 128, 3, 8192], P(None, ('grp', 'dp'), None, 'tp'), parts along dimension 1, may hold values from -6 to 6
- ssm_state: float32 [2, 128, 64, 64, 128], P(None, ('grp', 'dp'), 'tp'), parts along dimension 1, may hold values from -2 to 2
Outputs:
- mixed_out: bfloat16 [128, 4096], P('grp', 'dp'), parts along dimension 0
- conv_new: bfloat16 [2, 128, 3, 8192], P(None, ('grp', 'dp'), None, 'tp'), parts along dimension 1
- ssm_new: float32 [2, 128, 64, 64, 128], P(None, ('grp', 'dp'), 'tp'), parts along dimension 1
The draws below stay inside these ranges and needn't reach their ends.
There are 2 independent parts, one for each index of `grp`. The reference program is written for one: setup_inputs(seed, part) draws one part's arguments, and reference() takes and returns one part's arrays. A program takes and returns all parts, laid end to end along the dimension named above; an argument that names none is the same for every part. Nothing has to cross between parts.
Inputs may be any that keep to these rules, and one draw needn't show every extreme that they name: `lengths`: each part has at least one sequence of length 24.
All inputs are finite; a program needn't handle non-finite values.
Results may differ from the reference program's by a relative error of at most 0.012.
Values may be sent and summed in bfloat16 or wider, within the bound.
A program may use at most 128 MiB of HBM per device.

```python
import jax
import jax.numpy as jnp
from jax import lax

D = 4096
HEADS = 64
GROUPS = 16
HEAD_DIM = 64
STATE = 128
CONV_W = 4
LAYERS = 2
BATCH = 64
SSD_W = 4096
CONV_DIM = 8192


def draw_tokens(key, part):
    first_key = jax.random.fold_in(key, 11)
    second_key = jax.random.fold_in(key, 12)
    columns = 10.0 ** (jnp.arange(D, dtype=jnp.float32) / D - 0.5)
    rowscale = jnp.exp(jax.random.uniform(first_key, (BATCH,), jnp.float32, -1.1513, 1.1513))
    entries = jnp.clip(jax.random.normal(second_key, (BATCH, D), jnp.float32), -5.0, 5.0)
    return (entries * rowscale[:, None] * columns[None, :]).astype(jnp.bfloat16)


def draw_lengths(key, part):
    short_key = jax.random.fold_in(key, 21)
    pick_key = jax.random.fold_in(key, 22)
    long_key = jax.random.fold_in(key, 23)
    place_key = jax.random.fold_in(key, 24)
    short_len = jax.random.randint(short_key, (BATCH,), 1, 7, dtype=jnp.int32)
    picked = jax.random.randint(pick_key, (BATCH,), 0, 8, dtype=jnp.int32) == 0
    long_len = jax.random.randint(long_key, (BATCH,), 12, 25, dtype=jnp.int32)
    chosen = jnp.where(picked, long_len, short_len)
    place = jax.random.randint(place_key, (), 0, BATCH, dtype=jnp.int32)
    return jnp.where(jnp.arange(BATCH, dtype=jnp.int32) == place, jnp.int32(24), chosen).astype(jnp.int32)


def block_scale(rng, dims, cuts, smallest, top_value):
    def one(dim, blocks):
        heights = jax.random.uniform(jax.random.fold_in(jax.random.fold_in(rng, 6), dim), (blocks,), jnp.float32, smallest / len(cuts), top_value / len(cuts))
        return jnp.repeat(jnp.exp(heights), dims[dim] // blocks).reshape((-1,) + (1,) * (len(dims) - dim - 1))

    factor_of = one(*cuts[0])
    for cut in cuts[1:]:
        factor_of = factor_of * one(*cut)
    return factor_of


def bell_draw(stream_key, shape, spread, limit, cuts=(), kind=jnp.bfloat16):
    drawn = spread * jax.random.normal(stream_key, shape, jnp.float32)
    if cuts:
        drawn = drawn * block_scale(stream_key, shape, cuts, -0.22, 0.18)
    return jnp.clip(drawn, -limit, limit).astype(kind)


def setup_inputs(seed: int = 0, part: int = 0) -> dict:
    arg_keys = jax.random.split(jax.random.key(seed), 17)
    own_keys = jax.random.split(jax.random.fold_in(arg_keys[16], part), 17)
    return {
        "tokens": draw_tokens(jax.random.fold_in(jax.random.fold_in(arg_keys[16], part), 71), part),
        "lengths": draw_lengths(jax.random.fold_in(jax.random.fold_in(arg_keys[16], part), 71), part),
        "norm_gain": jnp.clip(1.0 + 0.18 * jax.random.normal(arg_keys[2], (LAYERS, D), jnp.float32), 0.1, 1.9),
        "w_z": bell_draw(arg_keys[3], (LAYERS, D, SSD_W), D ** -0.5, 0.09375, ((1, 4), (2, 4))),
        "w_x": bell_draw(arg_keys[4], (LAYERS, D, SSD_W), D ** -0.5, 0.09375, ((1, 4), (2, 4))),
        "w_b": bell_draw(arg_keys[5], (LAYERS, D, GROUPS * STATE), D ** -0.5, 0.09375, ((1, 4), (2, 4))),
        "w_c": bell_draw(arg_keys[6], (LAYERS, D, GROUPS * STATE), D ** -0.5, 0.09375, ((1, 4), (2, 4))),
        "w_dt": bell_draw(arg_keys[7], (LAYERS, D, HEADS), D ** -0.5, 0.09375, ((1, 4),)),
        "conv_weight": bell_draw(arg_keys[8], (LAYERS, CONV_W, CONV_DIM), 0.5, 3.0, ((2, 4),)),
        "dt_bias": jnp.clip(-6.0 + 4.5 * jax.random.uniform(arg_keys[9], (LAYERS, HEADS), jnp.float32) ** block_scale(arg_keys[9], (LAYERS, HEADS), ((1, 4),), -0.2, 0.2), -6.0, -1.5),
        "a_log": jnp.clip(2.77 * jax.random.uniform(arg_keys[10], (LAYERS, HEADS), jnp.float32) ** block_scale(arg_keys[10], (LAYERS, HEADS), ((1, 4),), -0.2, 0.2), 0.0, 2.77),
        "d_skip": jnp.clip(1.0 + 0.18 * jax.random.normal(arg_keys[11], (LAYERS, HEADS), jnp.float32), 0.1, 1.9),
        "out_gain": jnp.clip(1.0 + 0.18 * jax.random.normal(arg_keys[12], (LAYERS, SSD_W), jnp.float32), 0.1, 1.9),
        "w_out": bell_draw(arg_keys[13], (LAYERS, SSD_W, D), SSD_W ** -0.5, 0.09375, ((1, 4), (2, 4))),
        "conv_state": bell_draw(own_keys[14], (LAYERS, BATCH, CONV_W - 1, CONV_DIM), 1.0, 6.0, ((1, 4), (3, 4))),
        "ssm_state": bell_draw(own_keys[15], (LAYERS, BATCH, HEADS, HEAD_DIM, STATE), 0.15, 2.0, ((1, 4), (2, 4)), jnp.float32),
    }


EPSILON = 1e-06

def one_block(stream, lengths, gain, w_z, w_x, w_b, w_c, w_dt, taps_weight, dt_bias, a_log, d_skip, out_gain, w_out, conv_past, ssm_past):
    batch_rows = stream.shape[0]
    per_group = HEADS // GROUPS
    width_x = per_group * HEAD_DIM
    wide = stream.astype(jnp.float32)
    inverse = lax.rsqrt(lax.optimization_barrier(jnp.mean(wide * wide, axis=-1)) + EPSILON)[:, None]
    normed = (wide * gain).astype(jnp.bfloat16)
    gating = (jnp.dot(normed, w_z, preferred_element_type=jnp.float32) * inverse).astype(jnp.bfloat16)
    values = (jnp.dot(normed, w_x, preferred_element_type=jnp.float32) * inverse).astype(jnp.bfloat16)
    writes = (jnp.dot(normed, w_b, preferred_element_type=jnp.float32) * inverse).astype(jnp.bfloat16)
    reads = (jnp.dot(normed, w_c, preferred_element_type=jnp.float32) * inverse).astype(jnp.bfloat16)
    step_raw = jnp.dot(normed, w_dt, preferred_element_type=jnp.float32) * inverse
    current = jnp.concatenate([values.reshape(batch_rows, GROUPS, width_x), writes.reshape(batch_rows, GROUPS, STATE), reads.reshape(batch_rows, GROUPS, STATE)], axis=-1).reshape(batch_rows, CONV_DIM)
    offsets = jnp.arange(CONV_W - 1, dtype=jnp.int32)
    alive = lengths[:, None] + offsets[None, :] >= CONV_W
    history = jnp.where(alive[:, :, None], conv_past, jnp.zeros_like(conv_past))
    conv_next = jnp.concatenate([history[:, 1:], current[:, None]], axis=1)
    summed = current.astype(jnp.float32) * taps_weight[CONV_W - 1].astype(jnp.float32)
    for tap_at in range(CONV_W - 1):
        summed = summed + history[:, tap_at].astype(jnp.float32) * taps_weight[tap_at].astype(jnp.float32)
    activated = jax.nn.silu(summed).reshape(batch_rows, GROUPS, width_x + 2 * STATE)
    head_in = activated[:, :, :width_x].reshape(batch_rows, GROUPS, per_group, HEAD_DIM)
    write_keys = activated[:, :, width_x:width_x + STATE]
    read_keys = activated[:, :, width_x + STATE:]
    step = jax.nn.softplus(step_raw + dt_bias).reshape(batch_rows, GROUPS, per_group)
    decay = jnp.exp(-jnp.exp(a_log).reshape(GROUPS, per_group) * step)
    carried = lengths >= 2
    before = ssm_past.reshape(batch_rows, GROUPS, per_group, HEAD_DIM, STATE)
    before = jnp.where(carried[:, None, None, None, None], before, jnp.zeros_like(before))
    state_next = decay[..., None, None] * before + (step[..., None] * head_in)[..., None] * write_keys[:, :, None, None, :]
    readout = jnp.einsum('bghpn,bgn->bghp', state_next, read_keys, precision=lax.Precision.HIGHEST)
    readout = readout + d_skip.reshape(GROUPS, per_group)[..., None] * head_in
    gated = readout.reshape(batch_rows, GROUPS, width_x) * jax.nn.silu(gating.astype(jnp.float32).reshape(batch_rows, GROUPS, width_x))
    gated = gated * lax.rsqrt(lax.optimization_barrier(jnp.mean(gated * gated, axis=-1, keepdims=True)) + EPSILON) * out_gain.reshape(GROUPS, width_x)
    mixed = gated.reshape(batch_rows, SSD_W).astype(jnp.bfloat16)
    stream_next = (wide + jnp.dot(mixed, w_out, preferred_element_type=jnp.float32)).astype(jnp.bfloat16)
    return (stream_next, conv_next, state_next.reshape(batch_rows, HEADS, HEAD_DIM, STATE))

def reference(tokens, lengths, norm_gain, w_z, w_x, w_b, w_c, w_dt, conv_weight, dt_bias, a_log, d_skip, out_gain, w_out, conv_state, ssm_state):
    stream = tokens
    conv_list = []
    ssm_list = []
    for layer_at in range(LAYERS):
        stream, conv_next, state_next = one_block(stream, lengths, norm_gain[layer_at], w_z[layer_at], w_x[layer_at], w_b[layer_at], w_c[layer_at], w_dt[layer_at], conv_weight[layer_at], dt_bias[layer_at], a_log[layer_at], d_skip[layer_at], out_gain[layer_at], w_out[layer_at], conv_state[layer_at], ssm_state[layer_at])
        conv_list.append(conv_next)
        ssm_list.append(state_next)
    return (stream, jnp.stack(conv_list), jnp.stack(ssm_list))
```

```python
import functools

import jax
import jax.numpy as jnp
from jax import lax
from jax.experimental import pallas as pl
from jax.experimental.pallas import tpu as pltpu
from jax.sharding import PartitionSpec as P

D = 4096
HEADS = 64
GROUPS = 16
HEAD_DIM = 64
STATE = 128
CONV_W = 4
PER_GROUP = HEADS // GROUPS
WIDTH_X = PER_GROUP * HEAD_DIM
GROUP_W = WIDTH_X + 2 * STATE
EPSILON = 1e-06
MESH = pl.DeviceIdType.MESH
BF16 = jnp.bfloat16
F32 = jnp.float32


SCOPE = []


def mark(name):
    if SCOPE:
        SCOPE.pop().__exit__(None, None, None)
    if name:
        scope = jax.named_scope("m:" + name)
        scope.__enter__()
        SCOPE.append(scope)


def silu(t):
    return t / (1.0 + jnp.exp(-t))


def block_kernel(
    nd, nt,
    tokens_hbm, lens_hbm, gain_hbm, bias_hbm, alog_hbm, skip_hbm, ogain_hbm, taps_hbm, conv_hbm,
    wz_hbm, wx_hbm, wb_hbm, wc_hbm, wdt_hbm, wo_hbm, state_hbm,
    out_ref, kept_ref, state,
    tokens_ref, lens_ref, gain_ref, bias_ref, alog_ref, skip_ref, ogain_ref, taps_ref, conv_ref,
    wz, wx, wb, wc, wdt, wo,
    snd_e, snd_x, snd_b, snd_c, snd_z,
    rcv_e, rcv_x, rcv_b, rcv_c, rcv_z,
    mixes, snd_o, rcv_o, stream, normed_s, rk_s, y_s, wk_s, cols_s,
    w_sem, st_sem, in_sem, dps, dpr, ags, agr, rss, rsr, tgs, tgr,
):
    dp = lax.axis_index("dp")
    tp = lax.axis_index("tp")
    layers = gain_ref.shape[0]
    seqs = lens_ref.shape[1]
    batch = nd * seqs
    rows = batch // nt
    dloc = gain_ref.shape[1]
    width = wx.shape[2]
    lgroups = width // WIDTH_X

    pairs = ((wdt_hbm, wdt), (wx_hbm, wx), (wb_hbm, wb), (wc_hbm, wc), (wz_hbm, wz), (wo_hbm, wo))

    def weight(layer, at):
        src, dst = pairs[at]
        return pltpu.make_async_copy(src.at[layer], dst.at[layer], w_sem.at[layer, at])

    def states(layer):
        return pltpu.make_async_copy(state_hbm.at[layer], state.at[layer], st_sem.at[layer])

    mark("start")
    arrivals = [
        pltpu.make_async_copy(src, dst, in_sem.at[i])
        for i, (src, dst) in enumerate((
            (tokens_hbm, tokens_ref), (gain_hbm, gain_ref), (lens_hbm, lens_ref),
            (bias_hbm, bias_ref), (alog_hbm, alog_ref), (skip_hbm, skip_ref),
            (ogain_hbm, ogain_ref), (taps_hbm, taps_ref), (conv_hbm, conv_ref),
        ))
    ]
    for copy in arrivals[:8]:
        copy.start()
    for at in range(5):
        weight(0, at).start()
    arrivals[8].start()

    mark("barrier")
    barrier = pltpu.get_barrier_semaphore()
    for k in range(1, nd):
        pl.semaphore_signal(
            barrier, inc=1, device_id={"dp": lax.rem(dp + k, nd)}, device_id_type=MESH
        )
    for k in range(1, nt):
        pl.semaphore_signal(
            barrier, inc=1, device_id={"tp": lax.rem(tp + k, nt)}, device_id_type=MESH
        )
    pl.semaphore_wait(barrier, nd - 1 + nt - 1)

    def scatter(layer, snd, rcv, at):
        copies = []
        for k in range(1, nd):
            peer = lax.rem(dp + k, nd)
            copy = pltpu.make_async_remote_copy(
                src_ref=snd.at[layer, peer],
                dst_ref=rcv.at[layer, k - 1],
                send_sem=dps.at[layer, at, k - 1],
                recv_sem=dpr.at[layer, at, k - 1],
                device_id={"dp": peer},
                device_id_type=MESH,
            )
            copy.start()
            copies.append(copy)
        return copies

    def gathered(copies, layer, snd, rcv):
        for copy in copies:
            copy.wait_recv()
        total = snd[layer, dp].astype(F32)
        for k in range(nd - 1):
            total = total + rcv[layer, k].astype(F32)
        return total

    mark("prep")
    for copy in arrivals[:8]:
        copy.wait()
    heads_all = wdt.shape[1]
    lheads = bias_ref.shape[1]

    def expand(values, offset):
        count = values.shape[1]
        head = lax.broadcasted_iota(jnp.int32, (count, width), 0)
        lane = lax.broadcasted_iota(jnp.int32, (count, width), 1)
        pick = jnp.where(head == lane // HEAD_DIM + offset, 1.0, 0.0).astype(F32)
        return jnp.dot(
            values, pick, preferred_element_type=F32, precision=lax.Precision.HIGHEST
        )

    bias = expand(bias_ref[...], 0)
    rate = jnp.exp(expand(alog_ref[...], 0))
    skip = expand(skip_ref[...], 0)
    spread = jnp.broadcast_to(lens_ref[...].astype(F32), (seqs, seqs))
    diagonal = lax.broadcasted_iota(jnp.int32, (seqs, seqs), 0) == lax.broadcasted_iota(
        jnp.int32, (seqs, seqs), 1
    )
    lens = jnp.sum(jnp.where(diagonal, spread, 0.0), axis=1, keepdims=True)
    pending = []

    for layer in range(layers):
        mark("norm")
        source = tokens_ref if layer == 0 else stream.at[layer - 1]
        wide = source[...].astype(F32).reshape(batch, dloc)
        squares = jnp.sum(wide * wide, axis=-1, keepdims=True)
        normed_s[...] = (wide * gain_ref[layer : layer + 1, :]).astype(BF16)

        def project(w_ref, snd, layer=layer):
            n = w_ref.shape[2]
            tile = min(n, 1024)

            def step(j, carry):
                cols = pl.ds(pl.multiple_of(j * tile, tile), tile)
                part = jnp.dot(
                    normed_s[...], w_ref[layer, :, cols], preferred_element_type=F32
                )
                snd[layer, :, :, cols] = part.reshape(nd, seqs, tile).astype(snd.dtype)
                return carry

            lax.fori_loop(0, n // tile, step, 0)

        mark("proj_dt")
        weight(layer, 0).wait()
        part_dt = lax.dot_general(
            normed_s[...], wdt[layer], (((1,), (1,)), ((), ())), preferred_element_type=F32
        )
        snd_e[layer] = jnp.concatenate(
            [part_dt, jnp.broadcast_to(squares, (batch, heads_all))], axis=1
        ).reshape(nd, seqs, 2 * heads_all)
        mark("proj_x")
        weight(layer, 1).wait()
        project(wx, snd_x)
        copies_x = scatter(layer, snd_x, rcv_x, 1)
        copies_e = scatter(layer, snd_e, rcv_e, 0)
        mark("proj_b")
        weight(layer, 2).wait()
        project(wb, snd_b)
        copies_b = scatter(layer, snd_b, rcv_b, 2)
        mark("proj_c")
        weight(layer, 3).wait()
        project(wc, snd_c)
        copies_c = scatter(layer, snd_c, rcv_c, 3)
        mark("proj_z")
        weight(layer, 4).wait()
        if layer == 0:
            states(0).start()
            weight(0, 5).start()
        project(wz, snd_z)
        copies_z = scatter(layer, snd_z, rcv_z, 4)
        if layer + 1 < layers:
            for at in range(6):
                weight(layer + 1, at).start()
            states(layer + 1).start()

        mark("wait_e")
        extra = gathered(copies_e, layer, snd_e, rcv_e)
        inverse = lax.rsqrt(extra[:, heads_all : heads_all + 1] / D + EPSILON)
        raw = expand(extra[:, 0:heads_all] * inverse, tp * lheads)
        softin = raw + bias[layer : layer + 1, :]
        step = jnp.maximum(softin, 0.0) + jnp.log1p(jnp.exp(-jnp.abs(softin)))
        decay = jnp.exp(-rate[layer : layer + 1, :] * step)
        decay = jnp.where(lens >= 2, decay, 0.0)

        mark("wait_xbc")
        values = (gathered(copies_x, layer, snd_x, rcv_x) * inverse).astype(BF16)
        writes = (gathered(copies_b, layer, snd_b, rcv_b) * inverse).astype(BF16)
        reads = (gathered(copies_c, layer, snd_c, rcv_c) * inverse).astype(BF16)
        mark("conv")
        if layer == 0:
            arrivals[8].wait()
        pieces = []
        for g in range(lgroups):
            pieces.append(values[:, g * WIDTH_X : (g + 1) * WIDTH_X])
            pieces.append(writes[:, g * STATE : (g + 1) * STATE])
            pieces.append(reads[:, g * STATE : (g + 1) * STATE])
        current = jnp.concatenate(pieces, axis=1)
        kept_ref[layer, CONV_W - 2] = current
        summed = current.astype(F32) * taps_ref[
            layer, CONV_W - 1 : CONV_W, :
        ].astype(F32)
        for tap in range(CONV_W - 1):
            past = conv_ref[layer, tap].astype(F32)
            past = jnp.where(lens >= CONV_W - tap, past, 0.0)
            if tap >= 1:
                kept_ref[layer, tap - 1] = past.astype(BF16)
            summed = summed + past * taps_ref[layer, tap : tap + 1, :].astype(F32)
        active = silu(summed)
        head_in = jnp.concatenate(
            [active[:, g * GROUP_W : g * GROUP_W + WIDTH_X] for g in range(lgroups)], axis=1
        )
        wk = [
            active[:, g * GROUP_W + WIDTH_X : g * GROUP_W + WIDTH_X + STATE]
            for g in range(lgroups)
        ]
        rk = [active[:, g * GROUP_W + WIDTH_X + STATE : (g + 1) * GROUP_W] for g in range(lgroups)]
        stepx = step * head_in
        for g in range(lgroups):
            wk_s[g] = wk[g]
        rk_s[...] = jnp.concatenate(rk, axis=1)

        mark("wait_state")
        states(layer).wait()

        mark("readout")
        def read_eight(b, carry, layer=layer):
            at = pl.ds(pl.multiple_of(b * 8, 8), 8)
            keys = rk_s[at, :]
            lines = []
            for i in range(8):
                outs = []
                for g in range(lgroups):
                    row = keys[i : i + 1, g * STATE : (g + 1) * STATE]
                    lhs = jnp.broadcast_to(row, (16, STATE)).astype(BF16)
                    held = state[layer, b * 8 + i, g * PER_GROUP : (g + 1) * PER_GROUP]
                    held = held.reshape(WIDTH_X, STATE).astype(BF16)
                    res = lax.dot_general(
                        lhs, held, (((1,), (1,)), ((), ())), preferred_element_type=F32
                    )
                    outs.append(res[0:1])
                lines.append(jnp.concatenate(outs, axis=1))
            y_s[at, :] = jnp.concatenate(lines, axis=0)
            return carry

        lax.fori_loop(0, seqs // 8, read_eight, 0)
        mark("wait_z_gate")
        readout = decay * y_s[...] + skip[layer : layer + 1, :] * head_in
        gate = (gathered(copies_z, layer, snd_z, rcv_z) * inverse).astype(BF16).astype(F32)
        gate = silu(gate)
        mixed = []
        for g in range(lgroups):
            cols = slice(g * WIDTH_X, (g + 1) * WIDTH_X)
            cross = jnp.sum(wk[g] * rk[g], axis=-1, keepdims=True)
            gated = (readout[:, cols] + stepx[:, cols] * cross) * gate[:, cols]
            norm = lax.rsqrt(jnp.mean(gated * gated, axis=-1, keepdims=True) + EPSILON)
            mixed.append(gated * norm * ogain_ref[layer : layer + 1, cols])
        mixes[layer, dp] = jnp.concatenate(mixed, axis=1).astype(BF16)
        mark("send_m")
        copies_m = []
        for k in range(1, nd):
            copy = pltpu.make_async_remote_copy(
                src_ref=mixes.at[layer, dp],
                dst_ref=mixes.at[layer, dp],
                send_sem=ags.at[layer, k - 1],
                recv_sem=agr.at[layer, k - 1],
                device_id={"dp": lax.rem(dp + k, nd)},
                device_id_type=MESH,
            )
            copy.start()
            copies_m.append(copy)
        mark("update")
        cols_s[...] = jnp.concatenate(
            [stepx, decay, jnp.zeros((128 - 2 * seqs, width), F32)], axis=0
        ).T

        def update(h, carry, layer=layer):
            first = pl.multiple_of(h * HEAD_DIM, HEAD_DIM)
            adds = cols_s[pl.ds(first, HEAD_DIM), :]
            keeps = cols_s[pl.ds(first, 8), :]
            keys = wk_s[h // PER_GROUP]
            for i in range(seqs):
                keep = jnp.broadcast_to(keeps[:, seqs + i : seqs + i + 1], (8, STATE))
                add = jnp.broadcast_to(adds[:, i : i + 1], (HEAD_DIM, STATE)) * keys[i : i + 1]
                held = state[layer, i, h].reshape(HEAD_DIM // 8, 8, STATE)
                new = held * keep[None] + add.reshape(HEAD_DIM // 8, 8, STATE)
                state[layer, i, h] = new.reshape(HEAD_DIM, STATE)
            return carry

        lax.fori_loop(0, lheads // 2, update, 0)
        weight(layer, 5).wait()
        mark("wait_m")
        for copy in copies_m:
            copy.wait_recv()

        mark("outproj")
        tile = min(dloc, 1024)

        def project_out(j, carry, layer=layer):
            cols = pl.ds(pl.multiple_of(j * tile, tile), tile)
            lhs = mixes[layer].reshape(batch, width)
            part = jnp.dot(lhs, wo[layer, :, cols], preferred_element_type=F32)
            snd_o[layer, :, :, cols] = part.reshape(nt, rows, tile).astype(BF16)
            return carry

        lax.fori_loop(0, dloc // tile, project_out, 0)
        mark("send_o_wait")
        copies_o = []
        for k in range(1, nt):
            peer = lax.rem(tp + k, nt)
            copy = pltpu.make_async_remote_copy(
                src_ref=snd_o.at[layer, peer],
                dst_ref=rcv_o.at[layer, k - 1],
                send_sem=rss.at[layer, k - 1],
                recv_sem=rsr.at[layer, k - 1],
                device_id={"tp": peer},
                device_id_type=MESH,
            )
            copy.start()
            copies_o.append(copy)
        lax.fori_loop(lheads // 2, lheads * 3 // 4, update, 0)
        total = source[tp].astype(F32) + snd_o[layer, tp].astype(F32)
        for k in range(nt - 1):
            copies_o[k].wait_recv()
            total = total + rcv_o[layer, k].astype(F32)
        mark("send_s_wait")
        stream[layer, tp] = total.astype(BF16)
        copies_s = []
        for k in range(1, nt):
            copy = pltpu.make_async_remote_copy(
                src_ref=stream.at[layer, tp],
                dst_ref=stream.at[layer, tp],
                send_sem=tgs.at[layer, k - 1],
                recv_sem=tgr.at[layer, k - 1],
                device_id={"tp": lax.rem(tp + k, nt)},
                device_id_type=MESH,
            )
            copy.start()
            copies_s.append(copy)
        lax.fori_loop(lheads * 3 // 4, lheads, update, 0)
        for copy in copies_s:
            copy.wait_recv()
        mark("end")
        for group in (copies_e, copies_x, copies_b, copies_c, copies_z, copies_m, copies_o, copies_s):
            pending.extend(group)

    mark("final")
    out_ref[...] = stream[layers - 1]
    for copy in pending:
        copy.wait_send()
    mark(None)


def store_kernel(stream_ref, kept_ref, state_ref, out_ref, conv_ref, new_ref, sem):
    layers, seqs = state_ref.shape[0:2]
    count = 2
    copies = [
        pltpu.make_async_copy(stream_ref, out_ref, sem.at[0]),
        pltpu.make_async_copy(kept_ref, conv_ref, sem.at[1]),
    ]
    for layer in range(layers):
        for first in range(0, seqs, count):
            rows = pl.ds(first, count)
            copies.append(
                pltpu.make_async_copy(
                    state_ref.at[layer, rows], new_ref.at[layer, rows], sem.at[len(copies)]
                )
            )
    for copy in copies:
        copy.start()
    for copy in copies:
        copy.wait()


def body(
    nd, nt,
    tokens, lengths, norm_gain, w_z, w_x, w_b, w_c, w_dt, conv_weight,
    dt_bias, a_log, d_skip, out_gain, w_out, conv_state, ssm_state,
):
    layers = w_z.shape[0]
    batch, dloc = tokens.shape
    seqs = lengths.shape[0]
    rows = batch // nt
    width = w_x.shape[2]
    keys = w_b.shape[2]
    turned = jnp.swapaxes(w_dt, 1, 2)
    conv_w = conv_weight.shape[2]
    heads_all = turned.shape[1]
    vmem = pl.BlockSpec(memory_space=pltpu.VMEM)
    hbm = pl.BlockSpec(memory_space=pltpu.HBM)
    dma = pltpu.SemaphoreType.DMA
    sizes = (width, keys, keys, width)
    past = jnp.transpose(conv_state, (0, 2, 1, 3))
    stream, kept, new = pl.pallas_call(
        functools.partial(block_kernel, nd, nt),
        out_shape=(
            pltpu.VMEM((nt, rows, dloc), BF16),
            pltpu.VMEM((layers, CONV_W - 1, seqs, conv_w), BF16),
            pltpu.VMEM(ssm_state.shape, F32),
        ),
        in_specs=[hbm] * 16,
        out_specs=[vmem] * 3,
        scratch_shapes=[
            pltpu.VMEM((nt, rows, dloc), BF16),
            pltpu.VMEM((1, seqs), jnp.int32),
            pltpu.VMEM(norm_gain.shape, F32),
            pltpu.VMEM(dt_bias.shape, F32),
            pltpu.VMEM(a_log.shape, F32),
            pltpu.VMEM(d_skip.shape, F32),
            pltpu.VMEM(out_gain.shape, F32),
            pltpu.VMEM(conv_weight.shape, BF16),
            pltpu.VMEM(past.shape, BF16),
            pltpu.VMEM(w_z.shape, BF16),
            pltpu.VMEM(w_x.shape, BF16),
            pltpu.VMEM(w_b.shape, BF16),
            pltpu.VMEM(w_c.shape, BF16),
            pltpu.VMEM(turned.shape, BF16),
            pltpu.VMEM(w_out.shape, BF16),
            pltpu.VMEM((layers, nd, seqs, 2 * heads_all), F32),
            *[pltpu.VMEM((layers, nd, seqs, n), BF16) for n in sizes],
            pltpu.VMEM((layers, nd - 1, seqs, 2 * heads_all), F32),
            *[pltpu.VMEM((layers, nd - 1, seqs, n), BF16) for n in sizes],
            pltpu.VMEM((layers, nd, seqs, width), BF16),
            pltpu.VMEM((layers, nt, rows, dloc), BF16),
            pltpu.VMEM((layers, nt - 1, rows, dloc), BF16),
            pltpu.VMEM((layers, nt, rows, dloc), BF16),
            pltpu.VMEM((batch, dloc), BF16),
            pltpu.VMEM((seqs, keys), F32),
            pltpu.VMEM((seqs, width), F32),
            pltpu.VMEM((width // WIDTH_X, seqs, STATE), F32),
            pltpu.VMEM((width, 128), F32),
            dma((layers, 6)),
            dma((layers,)),
            dma((9,)),
            dma((layers, 5, nd - 1)),
            dma((layers, 5, nd - 1)),
            dma((layers, nd - 1)),
            dma((layers, nd - 1)),
            dma((layers, nt - 1)),
            dma((layers, nt - 1)),
            dma((layers, nt - 1)),
            dma((layers, nt - 1)),
        ],
        compiler_params=pltpu.CompilerParams(
            collective_id=0, has_side_effects=True, vmem_limit_bytes=40 * 1024 * 1024
        ),
    )(
        tokens.reshape(nt, rows, dloc), lengths[None, :], norm_gain, dt_bias, a_log, d_skip,
        out_gain, conv_weight, past, w_z, w_x, w_b, w_c, turned, w_out, ssm_state,
    )
    mixed_out, conv_new, ssm_new = pl.pallas_call(
        store_kernel,
        out_shape=(
            jax.ShapeDtypeStruct(stream.shape, BF16),
            jax.ShapeDtypeStruct(kept.shape, BF16),
            jax.ShapeDtypeStruct(ssm_state.shape, F32),
        ),
        in_specs=[vmem] * 3,
        out_specs=[hbm] * 3,
        scratch_shapes=[dma((2 + layers * seqs // 2,))],
        compiler_params=pltpu.CompilerParams(vmem_limit_bytes=1024 * 1024),
    )(stream, kept, new)
    return mixed_out.reshape(batch, dloc), jnp.transpose(conv_new, (0, 2, 1, 3)), ssm_new


def solution(mesh):
    placed = (
        P("grp", "dp"),
        P(("grp", "dp")),
        P(None, "dp"),
        P(None, "dp", "tp"),
        P(None, "dp", "tp"),
        P(None, "dp", "tp"),
        P(None, "dp", "tp"),
        P(None, "dp", None),
        P(None, None, "tp"),
        P(None, "tp"),
        P(None, "tp"),
        P(None, "tp"),
        P(None, "tp"),
        P(None, "tp", "dp"),
        P(None, ("grp", "dp"), None, "tp"),
        P(None, ("grp", "dp"), "tp", None, None),
    )
    return jax.shard_map(
        functools.partial(body, mesh.shape["dp"], mesh.shape["tp"]),
        mesh=mesh,
        in_specs=placed,
        out_specs=(
            P("grp", "dp"),
            P(None, ("grp", "dp"), None, "tp"),
            P(None, ("grp", "dp"), "tp", None, None),
        ),
        check_vma=False,
    )
```

```python
import functools

import jax
import jax.numpy as jnp
from jax import lax
from jax.experimental import pallas as pl
from jax.experimental.pallas import tpu as pltpu
from jax.sharding import PartitionSpec as P

D = 4096
HEADS = 64
GROUPS = 16
HEAD_DIM = 64
STATE = 128
CONV_W = 4
PER_GROUP = HEADS // GROUPS
WIDTH_X = PER_GROUP * HEAD_DIM
GROUP_W = WIDTH_X + 2 * STATE
EPSILON = 1e-06
MESH = pl.DeviceIdType.MESH
BF16 = jnp.bfloat16
F32 = jnp.float32


SCOPE = []


def mark(name):
    if SCOPE:
        SCOPE.pop().__exit__(None, None, None)
    if name:
        scope = jax.named_scope("m:" + name)
        scope.__enter__()
        SCOPE.append(scope)


def silu(t):
    return t / (1.0 + jnp.exp(-t))


def block_kernel(
    nd, nt,
    tokens_hbm, lens_hbm, gain_hbm, bias_hbm, alog_hbm, skip_hbm, ogain_hbm, taps_hbm, conv_hbm,
    wz_hbm, wx_hbm, wb_hbm, wc_hbm, wdt_hbm, wo_hbm, state_hbm,
    out_ref, kept_ref, state,
    tokens_ref, lens_ref, gain_ref, bias_ref, alog_ref, skip_ref, ogain_ref, taps_ref, conv_ref,
    wz, wx, wb, wc, wdt, wo,
    snd_e, snd_c, snd_x, snd_b, snd_z,
    rcv_e, rcv_c,
    one_x, one_b, one_z,
    two_x, two_b, two_z,
    rcv_x, rcv_b, rcv_z,
    mixes, snd_o, rcv_o, stream, acc_e, acc_c, acc_x, acc_b, acc_z, past_s, rk_s, y_s, wk_s, cols_s,
    w_sem, st_sem, in_sem, ones, oner, twos, twor, fans, fanr, rss, rsr, tgs, tgr,
):
    dp = lax.axis_index("dp")
    tp = lax.axis_index("tp")
    nx = nd // 2
    core = lax.rem(dp, 2)
    chip = dp // 2
    partner = chip * 2 + 1 - core
    layers = gain_ref.shape[0]
    seqs = lens_ref.shape[1]
    batch = nd * seqs
    rows = batch // nt
    dloc = gain_ref.shape[1]
    width = wx.shape[2]
    lgroups = width // WIDTH_X
    tile = min(dloc, 256)
    tiles = dloc // tile

    pairs = ((wdt_hbm, wdt), (wc_hbm, wc), (wx_hbm, wx), (wb_hbm, wb), (wz_hbm, wz), (wo_hbm, wo))

    def weight(layer, at):
        src, dst = pairs[at]
        return pltpu.make_async_copy(src.at[layer], dst.at[layer], w_sem.at[layer, at])

    def states(layer):
        return pltpu.make_async_copy(state_hbm.at[layer], state.at[layer], st_sem.at[layer])

    mark("start")
    arrivals = [
        pltpu.make_async_copy(src, dst, in_sem.at[i])
        for i, (src, dst) in enumerate((
            (tokens_hbm, tokens_ref), (gain_hbm, gain_ref), (lens_hbm, lens_ref),
            (bias_hbm, bias_ref), (alog_hbm, alog_ref), (skip_hbm, skip_ref),
            (ogain_hbm, ogain_ref), (taps_hbm, taps_ref), (conv_hbm, conv_ref),
        ))
    ]
    for copy in arrivals[:2]:
        copy.start()
    for at in range(5):
        weight(0, at).start()
    for copy in arrivals[2:]:
        copy.start()

    mark("barrier")
    barrier = pltpu.get_barrier_semaphore()
    for k in range(1, nd):
        pl.semaphore_signal(
            barrier, inc=1, device_id={"dp": lax.rem(dp + k, nd)}, device_id_type=MESH
        )
    for k in range(1, nt):
        pl.semaphore_signal(
            barrier, inc=1, device_id={"tp": lax.rem(tp + k, nt)}, device_id_type=MESH
        )

    streams = (
        (snd_e, None, None, rcv_e), (snd_c, None, None, rcv_c), (snd_x, one_x, two_x, rcv_x),
        (snd_b, one_b, two_b, rcv_b), (snd_z, one_z, two_z, rcv_z),
    )
    pending = []
    peers = [(k, j) for k in [*range(1, nx), 0] for j in range(2) if k or j]

    def swap(layer, at):
        snd, one = streams[at][0:2]
        copy = pltpu.make_async_remote_copy(
            src_ref=snd.at[layer, 1 - core],
            dst_ref=one.at[layer],
            send_sem=ones.at[layer, at - 2],
            recv_sem=oner.at[layer, at - 2],
            device_id={"dp": partner},
            device_id_type=MESH,
        )
        copy.start()
        pending.append(copy)
        return copy

    def relay(layer, at, swapped):
        snd, one, two, rcv = streams[at]
        swapped.wait_recv()
        copies = []
        for k in range(1, nx):
            other = lax.rem(chip + k, nx)
            summed = snd[layer, core, other].astype(F32) + one[layer, other].astype(F32)
            two[layer, k - 1] = summed.astype(two.dtype)
            copy = pltpu.make_async_remote_copy(
                src_ref=two.at[layer, k - 1],
                dst_ref=rcv.at[layer, k - 1],
                send_sem=twos.at[layer, at - 2, k - 1],
                recv_sem=twor.at[layer, at - 2, k - 1],
                device_id={"dp": other * 2 + core},
                device_id_type=MESH,
            )
            copy.start()
            copies.append(copy)
        pending.extend(copies)
        return copies

    def fan_out(layer, at, source, target):
        for i, (k, j) in enumerate(peers):
            peer_chip, peer_core = lax.rem(chip + k, nx), lax.rem(core + j, 2)
            pltpu.make_async_remote_copy(
                src_ref=source(peer_core, peer_chip),
                dst_ref=target(i),
                send_sem=fans.at[layer, at],
                recv_sem=fanr.at[layer, at],
                device_id={"dp": peer_chip * 2 + peer_core},
                device_id_type=MESH,
            ).start()

    def fanned(layer, at, ref):
        return pltpu.make_async_remote_copy(
            src_ref=ref,
            dst_ref=ref,
            send_sem=fans.at[layer, at],
            recv_sem=fanr.at[layer, at],
            device_id={"dp": partner},
            device_id_type=MESH,
        )

    def spread_out(layer, at):
        snd, rcv = streams[at][0], streams[at][3]
        fan_out(layer, at, lambda c, x: snd.at[layer, c, x], lambda i: rcv.at[layer, i])
        pending.append(fanned(layer, at, rcv.at[layer]))
        return pending[-1]

    def collected(layer, at, copy):
        snd, rcv = streams[at][0], streams[at][3]
        copy.wait_recv()
        total = snd[layer, core, chip].astype(F32)
        for i in range(nd - 1):
            total = total + rcv[layer, i].astype(F32)
        return total

    def gathered(layer, at, copies):
        snd, one, two, rcv = streams[at]
        total = snd[layer, core, chip].astype(F32) + one[layer, chip].astype(F32)
        for k in range(nx - 1):
            copies[k].wait_recv()
            total = total + rcv[layer, k].astype(F32)
        return total

    def far_first(k):
        down = nt - 1 - k
        down = jnp.where(down > tp, down, down - 1)
        up = jnp.where(k < tp, k, k + 1)
        return jnp.where(2 * tp < nt, down, up)

    def tp_copy(src, dst, sems, layer, q, peer):
        return pltpu.make_async_remote_copy(
            src_ref=src,
            dst_ref=dst,
            send_sem=sems[0].at[layer],
            recv_sem=sems[1].at[layer, q],
            device_id={"tp": peer},
            device_id_type=MESH,
        )

    def send_sums(layer, q):
        for k in range(nt - 1):
            peer = far_first(k)
            slot = lax.rem(tp + nt - peer, nt) - 1
            tp_copy(
                snd_o.at[layer, q, peer], rcv_o.at[layer, q, slot], (rss, rsr), layer, q, peer
            ).start()

    def wait_sums(layer, q):
        held = rcv_o.at[layer, q]
        tp_copy(held, held, (rss, rsr), layer, q, 0).wait_recv()

    def send_rows(layer, q):
        mine = stream.at[layer, q, tp]
        for k in range(nt - 1):
            tp_copy(mine, mine, (tgs, tgr), layer, q, far_first(k)).start()

    def wait_rows(layer, q):
        held = stream.at[layer, q, 0 : nt - 1]
        tp_copy(held, held, (tgs, tgr), layer, q, 0).wait_recv()

    mark("prep")
    for copy in arrivals[:2]:
        copy.wait()
    states(0).start()
    weight(0, 5).start()
    heads_all = wdt.shape[1]
    lheads = bias_ref.shape[1]

    def expand(values, offset):
        count = values.shape[1]
        head = lax.broadcasted_iota(jnp.int32, (count, width), 0)
        lane = lax.broadcasted_iota(jnp.int32, (count, width), 1)
        pick = jnp.where(head == lane // HEAD_DIM + offset, 1.0, 0.0).astype(F32)
        return jnp.dot(
            values, pick, preferred_element_type=F32, precision=lax.Precision.HIGHEST
        )

    for layer in range(layers):
        mark("project")
        squares = None
        last = tiles - 1 if layer else 0
        for q in range(last + 1):
            if layer:
                wait_rows(layer - 1, q)
                size = tile
                wide = stream[layer - 1, q].astype(F32).reshape(batch, size)
            else:
                size = dloc
                wide = tokens_ref[...].astype(F32).reshape(batch, size)
            feats = slice(q * size, (q + 1) * size)
            square = jnp.sum(wide * wide, axis=-1, keepdims=True)
            squares = square if q == 0 else squares + square
            lhs = (wide * gain_ref[layer : layer + 1, feats]).astype(BF16)

            def store(part, snd):
                for d in range(nd):
                    snd[layer, d % 2, d // 2] = part[d * seqs : (d + 1) * seqs].astype(snd.dtype)

            def project(at, w_ref, acc, snd):
                if q == 0:
                    weight(layer, at).wait()
                part = jnp.dot(lhs, w_ref[layer, feats, :], preferred_element_type=F32)
                if q:
                    part = part + acc[...]
                if q < last:
                    acc[...] = part
                else:
                    store(part, snd)

            project(1, wc, acc_c, snd_c)
            if q == last and layer:
                copies_c = spread_out(layer, 1)
            if q == 0:
                weight(layer, 0).wait()
            part = lax.dot_general(
                lhs, wdt[layer, :, feats], (((1,), (1,)), ((), ())), preferred_element_type=F32
            )
            if q:
                part = part + acc_e[...]
            if q < last:
                acc_e[...] = part
            else:
                total = jnp.broadcast_to(squares, (batch, heads_all))
                store(jnp.concatenate([part, total], axis=1), snd_e)
                if layer:
                    copies_e = spread_out(layer, 0)
            project(2, wx, acc_x, snd_x)
            if q == last and layer:
                swap_x = swap(layer, 2)
            project(3, wb, acc_b, snd_b)
            if q == last:
                if layer == 0:
                    pl.semaphore_wait(barrier, nd - 1 + nt - 1)
                    copies_c = spread_out(layer, 1)
                    copies_e = spread_out(layer, 0)
                    swap_x = swap(layer, 2)
                swap_b = swap(layer, 3)
            project(4, wz, acc_z, snd_z)
            if q == last:
                swap_z = swap(layer, 4)
        mark("relay_xbz")
        copies_x = relay(layer, 2, swap_x)
        copies_b = relay(layer, 3, swap_b)
        copies_z = relay(layer, 4, swap_z)
        mark("history")
        if layer + 1 < layers:
            for at in range(6):
                weight(layer + 1, at).start()
            states(layer + 1).start()
        if layer == 0:
            for copy in arrivals[2:]:
                copy.wait()
            bias = expand(bias_ref[...], 0)
            rate = jnp.exp(expand(alog_ref[...], 0))
            skip = expand(skip_ref[...], 0)
            spread = jnp.broadcast_to(lens_ref[...].astype(F32), (seqs, seqs))
            diagonal = lax.broadcasted_iota(jnp.int32, (seqs, seqs), 0) == lax.broadcasted_iota(
                jnp.int32, (seqs, seqs), 1
            )
            lens = jnp.sum(jnp.where(diagonal, spread, 0.0), axis=1, keepdims=True)
        summed = None
        for tap in range(CONV_W - 1):
            past = conv_ref[layer, tap].astype(F32)
            past = jnp.where(lens >= CONV_W - tap, past, 0.0)
            if tap >= 1:
                kept_ref[layer, tap - 1] = past.astype(BF16)
            past = past * taps_ref[layer, tap : tap + 1, :].astype(F32)
            summed = past if tap == 0 else summed + past
        past_s[...] = summed

        def convolve(current, first, size, layer=layer):
            found = []
            for g in range(lgroups):
                cols = slice(g * GROUP_W + first, g * GROUP_W + first + size)
                part = current[:, g * size : (g + 1) * size]
                kept_ref[layer, CONV_W - 2, :, cols] = part
                tap = taps_ref[layer, CONV_W - 1 : CONV_W, cols].astype(F32)
                found.append(silu(part.astype(F32) * tap + past_s[:, cols]))
            return found

        if layer:
            mark("update3")
            lax.fori_loop(lheads * 3 // 4, lheads, functools.partial(update, layer=layer - 1), 0)
        mark("wait_e")
        extra = collected(layer, 0, copies_e)
        inverse = lax.rsqrt(extra[:, heads_all : heads_all + 1] / D + EPSILON)
        raw = expand(extra[:, 0:heads_all] * inverse, tp * lheads)
        softin = raw + bias[layer : layer + 1, :]
        step = jnp.maximum(softin, 0.0) + jnp.log1p(jnp.exp(-jnp.abs(softin)))
        decay = jnp.exp(-rate[layer : layer + 1, :] * step)
        decay = jnp.where(lens >= 2, decay, 0.0)

        mark("wait_c")
        reads = (collected(layer, 1, copies_c) * inverse).astype(BF16)
        rk = convolve(reads, WIDTH_X + STATE, STATE)
        rk_s[...] = jnp.concatenate(rk, axis=1)
        mark("wait_state")
        states(layer).wait()

        mark("readout")
        def read_eight(b, carry, layer=layer):
            at = pl.ds(pl.multiple_of(b * 8, 8), 8)
            keys = rk_s[at, :]
            lines = []
            for i in range(8):
                outs = []
                for g in range(lgroups):
                    row = keys[i : i + 1, g * STATE : (g + 1) * STATE]
                    lhs = jnp.broadcast_to(row, (16, STATE)).astype(BF16)
                    held = state[layer, b * 8 + i, g * PER_GROUP : (g + 1) * PER_GROUP]
                    held = held.reshape(WIDTH_X, STATE).astype(BF16)
                    res = lax.dot_general(
                        lhs, held, (((1,), (1,)), ((), ())), preferred_element_type=F32
                    )
                    outs.append(res[0:1])
                lines.append(jnp.concatenate(outs, axis=1))
            y_s[at, :] = jnp.concatenate(lines, axis=0)
            return carry

        lax.fori_loop(0, seqs // 8, read_eight, 0)
        mark("wait_xb")
        values = (gathered(layer, 2, copies_x) * inverse).astype(BF16)
        head_in = jnp.concatenate(convolve(values, 0, WIDTH_X), axis=1)
        stepx = step * head_in
        writes = (gathered(layer, 3, copies_b) * inverse).astype(BF16)
        wk = convolve(writes, WIDTH_X, STATE)
        for g in range(lgroups):
            wk_s[g] = wk[g]
        mark("wait_z_gate")
        readout = decay * y_s[...] + skip[layer : layer + 1, :] * head_in
        gate = (gathered(layer, 4, copies_z) * inverse).astype(BF16).astype(F32)
        gate = silu(gate)
        mixed = []
        for g in range(lgroups):
            cols = slice(g * WIDTH_X, (g + 1) * WIDTH_X)
            cross = jnp.sum(wk[g] * rk[g], axis=-1, keepdims=True)
            gated = (readout[:, cols] + stepx[:, cols] * cross) * gate[:, cols]
            norm = lax.rsqrt(jnp.mean(gated * gated, axis=-1, keepdims=True) + EPSILON)
            mixed.append(gated * norm * ogain_ref[layer : layer + 1, cols])
        mixes[layer, dp] = jnp.concatenate(mixed, axis=1).astype(BF16)
        mark("send_m")
        mine = mixes.at[layer, dp]
        fan_out(layer, 2, lambda c, x: mine, lambda i: mine)
        copy_m = fanned(layer, 2, mixes.at[layer, 0 : nd - 1])
        pending.append(copy_m)
        mark("update")
        cols_s[...] = jnp.concatenate(
            [stepx, decay, jnp.zeros((128 - 2 * seqs, width), F32)], axis=0
        ).T

        def update(h, carry, layer=layer):
            first = pl.multiple_of(h * HEAD_DIM, HEAD_DIM)
            adds = cols_s[pl.ds(first, HEAD_DIM), :]
            keeps = cols_s[pl.ds(first, 8), :]
            keys = wk_s[h // PER_GROUP]
            for i in range(seqs):
                keep = jnp.broadcast_to(keeps[:, seqs + i : seqs + i + 1], (8, STATE))
                add = jnp.broadcast_to(adds[:, i : i + 1], (HEAD_DIM, STATE)) * keys[i : i + 1]
                held = state[layer, i, h].reshape(HEAD_DIM // 8, 8, STATE)
                new = held * keep[None] + add.reshape(HEAD_DIM // 8, 8, STATE)
                state[layer, i, h] = new.reshape(HEAD_DIM, STATE)
            return carry

        lax.fori_loop(0, lheads // 2, update, 0)
        weight(layer, 5).wait()
        mark("wait_m")
        copy_m.wait_recv()

        mark("outproj")
        lhs = mixes[layer].reshape(batch, width)
        for q in range(tiles):
            feats = slice(q * tile, (q + 1) * tile)
            part = jnp.dot(lhs, wo[layer, :, feats], preferred_element_type=F32)
            snd_o[layer, q] = part.reshape(nt, rows, tile).astype(BF16)
            send_sums(layer, q)
        mark("update2")
        lax.fori_loop(lheads // 2, lheads * 3 // 4, update, 0)
        mark("wait_o")
        for q in range(tiles):
            if layer:
                total = stream[layer - 1, q, tp].astype(F32)
            else:
                total = tokens_ref[tp, :, q * tile : (q + 1) * tile].astype(F32)
            total = total + snd_o[layer, q, tp].astype(F32)
            wait_sums(layer, q)
            for k in range(nt - 1):
                total = total + rcv_o[layer, q, k].astype(F32)
            stream[layer, q, tp] = total.astype(BF16)
            send_rows(layer, q)
        if layer + 1 == layers:
            mark("update3")
            lax.fori_loop(lheads * 3 // 4, lheads, update, 0)

    mark("wait_s")
    for q in range(tiles):
        wait_rows(layers - 1, q)
        out_ref[:, :, q * tile : (q + 1) * tile] = stream[layers - 1, q]
    mark("final")
    for copy in pending:
        copy.wait_send()
    for layer in range(layers):
        for ref, sems in ((snd_o, (rss, rsr)), (stream, (tgs, tgr))):
            held = ref.at[layer, :, 0 : nt - 1]
            tp_copy(held, held, sems, layer, 0, 0).wait_send()
    mark(None)


def store_kernel(stream_ref, kept_ref, state_ref, out_ref, conv_ref, new_ref, sem):
    layers, seqs = state_ref.shape[0:2]
    count = 4
    for layer in range(layers):
        for first in range(0, seqs, count):
            rows = pl.ds(first, count)
            pltpu.make_async_copy(
                state_ref.at[layer, rows], new_ref.at[layer, rows], sem.at[0]
            ).start()
    copies = [
        pltpu.make_async_copy(stream_ref, out_ref, sem.at[1]),
        pltpu.make_async_copy(kept_ref, conv_ref, sem.at[2]),
    ]
    for copy in copies:
        copy.start()
    for copy in copies:
        copy.wait()
    pltpu.make_async_copy(state_ref, new_ref, sem.at[0]).wait()


def body(
    nd, nt,
    tokens, lengths, norm_gain, w_z, w_x, w_b, w_c, w_dt, conv_weight,
    dt_bias, a_log, d_skip, out_gain, w_out, conv_state, ssm_state,
):
    layers = w_z.shape[0]
    batch, dloc = tokens.shape
    seqs = lengths.shape[0]
    rows = batch // nt
    width = w_x.shape[2]
    keys = w_b.shape[2]
    turned = jnp.swapaxes(w_dt, 1, 2)
    conv_w = conv_weight.shape[2]
    heads_all = turned.shape[1]
    vmem = pl.BlockSpec(memory_space=pltpu.VMEM)
    hbm = pl.BlockSpec(memory_space=pltpu.HBM)
    dma = pltpu.SemaphoreType.DMA
    nx = nd // 2
    tile = min(dloc, 256)
    tiles = dloc // tile

    def parts(*lead):
        shapes = [(layers, *lead, seqs, n) for n in (2 * heads_all, keys, width, keys, width)]
        return [pltpu.VMEM(shape, BF16 if i else F32) for i, shape in enumerate(shapes)]

    past = jnp.transpose(conv_state, (0, 2, 1, 3))
    stream, kept, new = pl.pallas_call(
        functools.partial(block_kernel, nd, nt),
        out_shape=(
            pltpu.VMEM((nt, rows, dloc), BF16),
            pltpu.VMEM((layers, CONV_W - 1, seqs, conv_w), BF16),
            pltpu.VMEM(ssm_state.shape, F32),
        ),
        in_specs=[hbm] * 16,
        out_specs=[vmem] * 3,
        scratch_shapes=[
            pltpu.VMEM((nt, rows, dloc), BF16),
            pltpu.VMEM((1, seqs), jnp.int32),
            pltpu.VMEM(norm_gain.shape, F32),
            pltpu.VMEM(dt_bias.shape, F32),
            pltpu.VMEM(a_log.shape, F32),
            pltpu.VMEM(d_skip.shape, F32),
            pltpu.VMEM(out_gain.shape, F32),
            pltpu.VMEM(conv_weight.shape, BF16),
            pltpu.VMEM(past.shape, BF16),
            pltpu.VMEM(w_z.shape, BF16),
            pltpu.VMEM(w_x.shape, BF16),
            pltpu.VMEM(w_b.shape, BF16),
            pltpu.VMEM(w_c.shape, BF16),
            pltpu.VMEM(turned.shape, BF16),
            pltpu.VMEM(w_out.shape, BF16),
            *parts(2, nx),
            *parts(nd - 1)[:2],
            *parts(nx)[2:],
            *parts(max(nx - 1, 1))[2:],
            *parts(max(nx - 1, 1))[2:],
            pltpu.VMEM((layers, nd, seqs, width), BF16),
            *[pltpu.VMEM((layers, tiles, n, rows, tile), BF16) for n in (nt, nt - 1, nt)],
            *[pltpu.VMEM((batch, n), F32) for n in (heads_all, keys, width, keys, width)],
            pltpu.VMEM((seqs, conv_w), F32),
            pltpu.VMEM((seqs, keys), F32),
            pltpu.VMEM((seqs, width), F32),
            pltpu.VMEM((width // WIDTH_X, seqs, STATE), F32),
            pltpu.VMEM((width, 128), F32),
            dma((layers, 6)),
            dma((layers,)),
            dma((9,)),
            dma((layers, 3)),
            dma((layers, 3)),
            dma((layers, 3, max(nx - 1, 1))),
            dma((layers, 3, max(nx - 1, 1))),
            dma((layers, 3)),
            dma((layers, 3)),
            dma((layers,)),
            dma((layers, tiles)),
            dma((layers,)),
            dma((layers, tiles)),
        ],
        compiler_params=pltpu.CompilerParams(
            collective_id=0, has_side_effects=True, vmem_limit_bytes=40 * 1024 * 1024
        ),
    )(
        tokens.reshape(nt, rows, dloc), lengths[None, :], norm_gain, dt_bias, a_log, d_skip,
        out_gain, conv_weight, past, w_z, w_x, w_b, w_c, turned, w_out, ssm_state,
    )
    mixed_out, conv_new, ssm_new = pl.pallas_call(
        store_kernel,
        out_shape=(
            jax.ShapeDtypeStruct(stream.shape, BF16),
            jax.ShapeDtypeStruct(kept.shape, BF16),
            jax.ShapeDtypeStruct(ssm_state.shape, F32),
        ),
        in_specs=[vmem] * 3,
        out_specs=[hbm] * 3,
        scratch_shapes=[dma((3,))],
        compiler_params=pltpu.CompilerParams(vmem_limit_bytes=1024 * 1024),
    )(stream, kept, new)
    return mixed_out.reshape(batch, dloc), jnp.transpose(conv_new, (0, 2, 1, 3)), ssm_new


def solution(mesh):
    placed = (
        P("grp", "dp"),
        P(("grp", "dp")),
        P(None, "dp"),
        P(None, "dp", "tp"),
        P(None, "dp", "tp"),
        P(None, "dp", "tp"),
        P(None, "dp", "tp"),
        P(None, "dp", None),
        P(None, None, "tp"),
        P(None, "tp"),
        P(None, "tp"),
        P(None, "tp"),
        P(None, "tp"),
        P(None, "tp", "dp"),
        P(None, ("grp", "dp"), None, "tp"),
        P(None, ("grp", "dp"), "tp", None, None),
    )
    return jax.shard_map(
        functools.partial(body, mesh.shape["dp"], mesh.shape["tp"]),
        mesh=mesh,
        in_specs=placed,
        out_specs=(
            P("grp", "dp"),
            P(None, ("grp", "dp"), None, "tp"),
            P(None, ("grp", "dp"), "tp", None, None),
        ),
        check_vma=False,
    )
```

```python
import functools

import jax
import jax.numpy as jnp
from jax import lax
from jax.experimental import pallas as pl
from jax.experimental.pallas import tpu as pltpu
from jax.sharding import PartitionSpec as P

D = 4096
HEADS = 64
GROUPS = 16
HEAD_DIM = 64
STATE = 128
CONV_W = 4
PER_GROUP = HEADS // GROUPS
WIDTH_X = PER_GROUP * HEAD_DIM
GROUP_W = WIDTH_X + 2 * STATE
EPSILON = 1e-06
MESH = pl.DeviceIdType.MESH
BF16 = jnp.bfloat16
F32 = jnp.float32


SCOPE = []


def mark(name):
    if SCOPE:
        SCOPE.pop().__exit__(None, None, None)
    if name:
        scope = jax.named_scope("m:" + name)
        scope.__enter__()
        SCOPE.append(scope)


def silu(t):
    return t / (1.0 + jnp.exp(-t))


def block_kernel(
    nd, nt,
    tokens_hbm, lens_hbm, gain_hbm, bias_hbm, alog_hbm, skip_hbm, ogain_hbm, taps_hbm, conv_hbm,
    wz_hbm, wx_hbm, wb_hbm, wc_hbm, wdt_hbm, wo_hbm, state_hbm,
    out_ref, kept_ref, state,
    tokens_ref, lens_ref, gain_ref, bias_ref, alog_ref, skip_ref, ogain_ref, taps_ref, conv_ref,
    wz, wx, wb, wc, wdt, wo,
    snd_e, snd_c, snd_x, snd_b, snd_z,
    rcv_e, rcv_c,
    one_x, one_b, one_z,
    two_x, two_b, two_z,
    rcv_x, rcv_b, rcv_z,
    mixes, snd_o, rcv_o, stream, acc_e, acc_c, acc_x, acc_b, acc_z, past_s, wk_s, cols_s,
    w_sem, st_sem, in_sem, ones, oner, twos, twor, fans, fanr, rss, rsr, tgs, tgr,
):
    dp = lax.axis_index("dp")
    tp = lax.axis_index("tp")
    nx = nd // 2
    core = lax.rem(dp, 2)
    chip = dp // 2
    partner = chip * 2 + 1 - core
    layers = gain_ref.shape[0]
    seqs = lens_ref.shape[1]
    batch = nd * seqs
    half = batch // 2
    first_owner = nt // 2 - 1
    own = tp - first_owner
    owner = jnp.logical_and(own >= 0, own < 2)
    far = jnp.where(2 * tp < nt, 1, 0)
    dloc = gain_ref.shape[1]
    width = wx.shape[2]
    lgroups = width // WIDTH_X
    tile = min(dloc, 256)
    tiles = dloc // tile

    pairs = ((wdt_hbm, wdt), (wc_hbm, wc), (wx_hbm, wx), (wb_hbm, wb), (wz_hbm, wz), (wo_hbm, wo))

    def weight(layer, at):
        src, dst = pairs[at]
        return pltpu.make_async_copy(src.at[layer], dst.at[layer], w_sem.at[at if at < 5 else at + layer])

    def states(layer):
        return pltpu.make_async_copy(state_hbm.at[layer], state.at[layer], st_sem.at[layer])

    mark("start")
    arrivals = [
        pltpu.make_async_copy(src, dst, in_sem.at[i])
        for i, (src, dst) in enumerate((
            (tokens_hbm, tokens_ref), (gain_hbm, gain_ref), (lens_hbm, lens_ref),
            (bias_hbm, bias_ref), (alog_hbm, alog_ref), (skip_hbm, skip_ref),
            (ogain_hbm, ogain_ref), (taps_hbm, taps_ref), (conv_hbm, conv_ref),
        ))
    ]
    for copy in arrivals[:2]:
        copy.start()
    for at in range(5):
        weight(0, at).start()
    for copy in arrivals[2:]:
        copy.start()

    mark("barrier")
    barrier = pltpu.get_barrier_semaphore()
    for k in range(1, nd):
        pl.semaphore_signal(
            barrier, inc=1, device_id={"dp": lax.rem(dp + k, nd)}, device_id_type=MESH
        )
    for i in range(2):

        @pl.when(own != i)
        def greet(i=i):
            pl.semaphore_signal(
                barrier, inc=1, device_id={"tp": first_owner + i}, device_id_type=MESH
            )

    for peer in (*range(first_owner), *range(first_owner + 2, nt)):

        @pl.when(owner)
        def answer(peer=peer):
            pl.semaphore_signal(barrier, inc=1, device_id={"tp": peer}, device_id_type=MESH)


    def hear_all():
        @pl.when(owner)
        def heard_all():
            pl.semaphore_wait(barrier, nd - 1 + nt - 1)

        @pl.when(jnp.logical_not(owner))
        def heard_owners():
            pl.semaphore_wait(barrier, nd - 1 + 2)

    streams = (
        (snd_e, None, None, rcv_e), (snd_c, None, None, rcv_c), (snd_x, one_x, two_x, rcv_x),
        (snd_b, one_b, two_b, rcv_b), (snd_z, one_z, two_z, rcv_z),
    )
    flying = {}
    peers = [(k, j) for k in [*range(1, nx), 0] for j in range(2) if k or j]

    def settle(key, copies):
        for copy in flying.pop(key, ()):
            copy.wait_send()
        if copies:
            flying[key] = copies

    def swap(layer, at):
        snd, one = streams[at][0:2]
        copy = pltpu.make_async_remote_copy(
            src_ref=snd.at[layer, 1 - core],
            dst_ref=one.at[layer],
            send_sem=ones.at[at - 2],
            recv_sem=oner.at[at - 2],
            device_id={"dp": partner},
            device_id_type=MESH,
        )
        settle(("swap", at), [copy])
        copy.start()
        return copy

    def relay(layer, at, swapped):
        snd, one, two, rcv = streams[at]
        settle(("relay", at), [])
        swapped.wait_recv()
        copies = []
        for k in range(1, nx):
            other = lax.rem(chip + k, nx)
            summed = snd[layer, core, other].astype(F32) + one[layer, other].astype(F32)
            two[layer, k - 1] = summed.astype(two.dtype)
            copy = pltpu.make_async_remote_copy(
                src_ref=two.at[layer, k - 1],
                dst_ref=rcv.at[layer, k - 1],
                send_sem=twos.at[at - 2, k - 1],
                recv_sem=twor.at[at - 2, k - 1],
                device_id={"dp": other * 2 + core},
                device_id_type=MESH,
            )
            copy.start()
            copies.append(copy)
        flying["relay", at] = copies
        return copies

    def fan_out(at, ref, source, target):
        settle(("fan", at), [fanned(at, ref)])
        for i, (k, j) in enumerate(peers):
            peer_chip, peer_core = lax.rem(chip + k, nx), lax.rem(core + j, 2)
            pltpu.make_async_remote_copy(
                src_ref=source(peer_core, peer_chip),
                dst_ref=target(i),
                send_sem=fans.at[at],
                recv_sem=fanr.at[at],
                device_id={"dp": peer_chip * 2 + peer_core},
                device_id_type=MESH,
            ).start()

    def fanned(at, ref):
        return pltpu.make_async_remote_copy(
            src_ref=ref,
            dst_ref=ref,
            send_sem=fans.at[at],
            recv_sem=fanr.at[at],
            device_id={"dp": partner},
            device_id_type=MESH,
        )

    def spread_out(layer, at):
        snd, rcv = streams[at][0], streams[at][3]
        fan_out(at, rcv.at[layer], lambda c, x: snd.at[layer, c, x], lambda i: rcv.at[layer, i])
        return fanned(at, rcv.at[layer])

    def collected(layer, at, copy):
        snd, rcv = streams[at][0], streams[at][3]
        copy.wait_recv()
        total = snd[layer, core, chip].astype(F32)
        for i in range(nd - 1):
            total = total + rcv[layer, i].astype(F32)
        return total

    def gathered(layer, at, copies):
        snd, one, two, rcv = streams[at]
        total = snd[layer, core, chip].astype(F32) + one[layer, chip].astype(F32)
        for k in range(nx - 1):
            copies[k].wait_recv()
            total = total + rcv[layer, k].astype(F32)
        return total

    def far_first(k):
        down = nt - 1 - k
        down = jnp.where(down > tp, down, down - 1)
        up = jnp.where(k < tp, k, k + 1)
        return jnp.where(2 * tp < nt, down, up)

    def tp_copy(src, dst, send, recv, peer):
        return pltpu.make_async_remote_copy(
            src_ref=src,
            dst_ref=dst,
            send_sem=send,
            recv_sem=recv,
            device_id={"tp": peer},
            device_id_type=MESH,
        )

    def send_sums(layer, q):
        for i in (far, 1 - far):

            @pl.when(own != i)
            def send(i=i):
                peer = first_owner + i
                slot = lax.rem(tp + nt - peer, nt) - 1
                tp_copy(
                    snd_o.at[layer, q, i], rcv_o.at[layer, q, slot],
                    rss.at[i], rsr.at[q], peer,
                ).start()

    def sent_sums(layer):
        for i in range(2):

            @pl.when(own != i)
            def sent(i=i):
                held = snd_o.at[layer, :, i]
                tp_copy(held, held, rss.at[i], rsr.at[0], 0).wait_send()

    def sent_rows(layer):
        @pl.when(owner)
        def sent():
            held = rcv_o.at[layer]
            tp_copy(held, held, tgs.at[0], tgr.at[0, 0], 0).wait_send()

    def wait_sums(layer, q):
        held = rcv_o.at[layer, q]
        tp_copy(held, held, rss.at[0], rsr.at[q], 0).wait_recv()

    def send_rows(layer, q):
        mine = stream.at[layer, q, own]
        for k in range(nt - 1):
            tp_copy(mine, mine, tgs.at[0], tgr.at[q, own], far_first(k)).start()

    def wait_rows(layer, q):
        for i in range(2):

            @pl.when(own != i)
            def wait(i=i):
                held = stream.at[layer, q, i]
                tp_copy(held, held, tgs.at[0], tgr.at[q, i], 0).wait_recv()

    mark("prep")
    for copy in arrivals[:2]:
        copy.wait()
    states(0).start()
    weight(0, 5).start()
    heads_all = wdt.shape[1]
    lheads = bias_ref.shape[1]

    def expand(values, offset):
        count = values.shape[1]
        head = lax.broadcasted_iota(jnp.int32, (count, width), 0)
        lane = lax.broadcasted_iota(jnp.int32, (count, width), 1)
        pick = jnp.where(head == lane // HEAD_DIM + offset, 1.0, 0.0).astype(F32)
        return jnp.dot(
            values, pick, preferred_element_type=F32, precision=lax.Precision.HIGHEST
        )

    for layer in range(layers):
        mark("project")
        squares = None
        last = tiles - 1 if layer else 0
        for q in range(last + 1):
            if layer:
                wait_rows(layer - 1, q)
                size = tile
                wide = stream[layer - 1, q].astype(F32).reshape(batch, size)
            else:
                size = dloc
                wide = tokens_ref[...].astype(F32).reshape(batch, size)
            feats = slice(q * size, (q + 1) * size)
            square = jnp.sum(wide * wide, axis=-1, keepdims=True)
            squares = square if q == 0 else squares + square
            lhs = (wide * gain_ref[layer : layer + 1, feats]).astype(BF16)

            def store(part, snd):
                for d in range(nd):
                    snd[layer, d % 2, d // 2] = part[d * seqs : (d + 1) * seqs].astype(snd.dtype)

            def project(at, w_ref, acc, snd):
                if q == 0:
                    weight(layer, at).wait()
                part = jnp.dot(lhs, w_ref[layer, feats, :], preferred_element_type=F32)
                if q:
                    part = part + acc[...]
                if q < last:
                    acc[...] = part
                else:
                    store(part, snd)

            project(1, wc, acc_c, snd_c)
            if q == last and layer:
                copies_c = spread_out(layer, 1)
            if q == 0:
                weight(layer, 0).wait()
            part = lax.dot_general(
                lhs, wdt[layer, :, feats], (((1,), (1,)), ((), ())), preferred_element_type=F32
            )
            if q:
                part = part + acc_e[...]
            if q < last:
                acc_e[...] = part
            else:
                total = jnp.broadcast_to(squares, (batch, heads_all))
                store(jnp.concatenate([part, total], axis=1), snd_e)
                if layer == 0:
                    hear_all()
                    copies_c = spread_out(layer, 1)
                copies_e = spread_out(layer, 0)
            project(2, wx, acc_x, snd_x)
            if q == last:
                swap_x = swap(layer, 2)
            project(3, wb, acc_b, snd_b)
            if q == last:
                swap_b = swap(layer, 3)
            project(4, wz, acc_z, snd_z)
            if q == last:
                swap_z = swap(layer, 4)
        mark("relay_xbz")
        copies_x = relay(layer, 2, swap_x)
        copies_b = relay(layer, 3, swap_b)
        copies_z = relay(layer, 4, swap_z)
        mark("history")
        if layer + 1 < layers:
            for at in range(6):
                weight(layer + 1, at).start()
            states(layer + 1).start()
        if layer == 0:
            for copy in arrivals[2:]:
                copy.wait()
            bias = expand(bias_ref[...], 0)
            rate = jnp.exp(expand(alog_ref[...], 0))
            skip = expand(skip_ref[...], 0)
            spread = jnp.broadcast_to(lens_ref[...].astype(F32), (seqs, seqs))
            diagonal = lax.broadcasted_iota(jnp.int32, (seqs, seqs), 0) == lax.broadcasted_iota(
                jnp.int32, (seqs, seqs), 1
            )
            lens = jnp.sum(jnp.where(diagonal, spread, 0.0), axis=1, keepdims=True)
        summed = None
        for tap in range(CONV_W - 1):
            past = conv_ref[layer, tap].astype(F32)
            past = jnp.where(lens >= CONV_W - tap, past, 0.0)
            if tap >= 1:
                kept_ref[layer, tap - 1] = past.astype(BF16)
            past = past * taps_ref[layer, tap : tap + 1, :].astype(F32)
            summed = past if tap == 0 else summed + past
        past_s[...] = summed

        def convolve(current, first, size, layer=layer):
            found = []
            for g in range(lgroups):
                cols = slice(g * GROUP_W + first, g * GROUP_W + first + size)
                part = current[:, g * size : (g + 1) * size]
                kept_ref[layer, CONV_W - 2, :, cols] = part
                tap = taps_ref[layer, CONV_W - 1 : CONV_W, cols].astype(F32)
                found.append(silu(part.astype(F32) * tap + past_s[:, cols]))
            return found

        if layer:
            mark("update3")
            lax.fori_loop(lheads * 3 // 4, lheads, functools.partial(update, layer=layer - 1), 0)
        mark("wait_e")
        extra = collected(layer, 0, copies_e)
        inverse = lax.rsqrt(extra[:, heads_all : heads_all + 1] / D + EPSILON)
        raw = expand(extra[:, 0:heads_all] * inverse, tp * lheads)
        softin = raw + bias[layer : layer + 1, :]
        step = jnp.maximum(softin, 0.0) + jnp.log1p(jnp.exp(-jnp.abs(softin)))
        decay = jnp.exp(-rate[layer : layer + 1, :] * step)
        decay = jnp.where(lens >= 2, decay, 0.0)

        mark("wait_c")
        reads = (collected(layer, 1, copies_c) * inverse).astype(BF16)
        rk = convolve(reads, WIDTH_X + STATE, STATE)
        mark("wait_state")
        states(layer).wait()

        def read_eight(first, layer=layer):
            lines = []
            for i in range(first, first + 8):
                outs = []
                for g in range(lgroups):
                    row = rk[g][i : i + 1]
                    lhs = jnp.broadcast_to(row, (16, STATE)).astype(BF16)
                    held = state[layer, i, g * PER_GROUP : (g + 1) * PER_GROUP]
                    held = held.reshape(WIDTH_X, STATE).astype(BF16)
                    res = lax.dot_general(
                        lhs, held, (((1,), (1,)), ((), ())), preferred_element_type=F32
                    )
                    outs.append(res[0:1])
                lines.append(jnp.concatenate(outs, axis=1))
            return jnp.concatenate(lines, axis=0)

        mark("readout")
        found = [read_eight(first) for first in range(0, seqs, 8)]
        mark("wait_xb")
        values = (gathered(layer, 2, copies_x) * inverse).astype(BF16)
        head_in = jnp.concatenate(convolve(values, 0, WIDTH_X), axis=1)
        stepx = step * head_in
        writes = (gathered(layer, 3, copies_b) * inverse).astype(BF16)
        wk = convolve(writes, WIDTH_X, STATE)
        for g in range(lgroups):
            wk_s[g] = wk[g]
        mark("wait_z")
        gate = (gathered(layer, 4, copies_z) * inverse).astype(BF16).astype(F32)
        gate = silu(gate)
        for part_at in range(seqs // 8):
            at = slice(part_at * 8, part_at * 8 + 8)
            mark("gate")
            readout = decay[at] * found[part_at] + skip[layer : layer + 1, :] * head_in[at]
            mixed = []
            for g in range(lgroups):
                cols = slice(g * WIDTH_X, (g + 1) * WIDTH_X)
                cross = jnp.sum(wk[g][at] * rk[g][at], axis=-1, keepdims=True)
                gated = (readout[:, cols] + stepx[at, cols] * cross) * gate[at, cols]
                norm = lax.rsqrt(jnp.mean(gated * gated, axis=-1, keepdims=True) + EPSILON)
                mixed.append(gated * norm * ogain_ref[layer : layer + 1, cols])
            mixes[layer, part_at, dp] = jnp.concatenate(mixed, axis=1).astype(BF16)
            mine = mixes.at[layer, part_at, dp]
            others = mixes.at[layer, part_at, 0 : nd - 1]
            fan_out(2 + part_at, others, lambda c, x, mine=mine: mine, lambda i, mine=mine: mine)
        mark("update")
        cols_s[...] = jnp.concatenate(
            [stepx, decay, jnp.zeros((128 - 2 * seqs, width), F32)], axis=0
        ).T

        def update(h, carry, layer=layer):
            first = pl.multiple_of(h * HEAD_DIM, HEAD_DIM)
            adds = cols_s[pl.ds(first, HEAD_DIM), :]
            keeps = cols_s[pl.ds(first, 8), :]
            keys = wk_s[h // PER_GROUP]
            for i in range(seqs):
                keep = jnp.broadcast_to(keeps[:, seqs + i : seqs + i + 1], (8, STATE))
                add = jnp.broadcast_to(adds[:, i : i + 1], (HEAD_DIM, STATE)) * keys[i : i + 1]
                held = state[layer, i, h].reshape(HEAD_DIM // 8, 8, STATE)
                new = held * keep[None] + add.reshape(HEAD_DIM // 8, 8, STATE)
                state[layer, i, h] = new.reshape(HEAD_DIM, STATE)
            return carry

        lax.fori_loop(0, lheads // 2, update, 0)
        weight(layer, 5).wait()
        mark("wait_m")
        for part_at in range(seqs // 8):
            fanned(2 + part_at, mixes.at[layer, part_at, 0 : nd - 1]).wait_recv()

        mark("outproj")
        if layer:
            sent_sums(layer - 1)
            sent_rows(layer - 1)
        lhs = mixes[layer].reshape(batch, width)
        for q in range(tiles):
            feats = slice(q * tile, (q + 1) * tile)
            part = jnp.dot(lhs, wo[layer, :, feats], preferred_element_type=F32)
            part = jnp.concatenate(
                [
                    part[(j * nd + d) * 8 : (j * nd + d) * 8 + 8]
                    for d in range(nd)
                    for j in range(seqs // 8)
                ],
                axis=0,
            )
            snd_o[layer, q] = part.reshape(2, half, tile).astype(BF16)
            send_sums(layer, q)
        mark("update2")
        lax.fori_loop(lheads // 2, lheads * 3 // 4, update, 0)
        mark("wait_o")

        @pl.when(owner)
        def add_up(layer=layer):
            for q in range(tiles):
                if layer:
                    total = stream[layer - 1, q, own].astype(F32)
                else:
                    total = tokens_ref[own, :, q * tile : (q + 1) * tile].astype(F32)
                total = total + snd_o[layer, q, own].astype(F32)
                wait_sums(layer, q)
                for k in range(nt - 1):
                    total = total + rcv_o[layer, q, k].astype(F32)
                stream[layer, q, own] = total.astype(BF16)
                send_rows(layer, q)

        if layer + 1 == layers:
            mark("update3")
            lax.fori_loop(lheads * 3 // 4, lheads, update, 0)

    mark("wait_s")
    for q in range(tiles):
        wait_rows(layers - 1, q)
        out_ref[:, :, q * tile : (q + 1) * tile] = stream[layers - 1, q]
    mark("final")
    for key in list(flying):
        settle(key, [])
    sent_sums(layers - 1)
    sent_rows(layers - 1)
    mark(None)


def store_kernel(stream_ref, kept_ref, state_ref, out_ref, conv_ref, new_ref, sem):
    layers, seqs = state_ref.shape[0:2]
    count = 4
    for layer in range(layers):
        for first in range(0, seqs, count):
            rows = pl.ds(first, count)
            pltpu.make_async_copy(
                state_ref.at[layer, rows], new_ref.at[layer, rows], sem.at[0]
            ).start()
    copies = [
        pltpu.make_async_copy(stream_ref, out_ref, sem.at[1]),
        pltpu.make_async_copy(kept_ref, conv_ref, sem.at[2]),
    ]
    for copy in copies:
        copy.start()
    for copy in copies:
        copy.wait()
    pltpu.make_async_copy(state_ref, new_ref, sem.at[0]).wait()


def body(
    nd, nt,
    tokens, lengths, norm_gain, w_z, w_x, w_b, w_c, w_dt, conv_weight,
    dt_bias, a_log, d_skip, out_gain, w_out, conv_state, ssm_state,
):
    layers = w_z.shape[0]
    batch, dloc = tokens.shape
    seqs = lengths.shape[0]
    half = batch // 2
    width = w_x.shape[2]
    keys = w_b.shape[2]
    turned = jnp.swapaxes(w_dt, 1, 2)
    conv_w = conv_weight.shape[2]
    heads_all = turned.shape[1]
    vmem = pl.BlockSpec(memory_space=pltpu.VMEM)
    hbm = pl.BlockSpec(memory_space=pltpu.HBM)
    dma = pltpu.SemaphoreType.DMA
    nx = nd // 2
    tile = min(dloc, 256)
    tiles = dloc // tile

    def parts(*lead):
        shapes = [(layers, *lead, seqs, n) for n in (2 * heads_all, keys, width, keys, width)]
        return [pltpu.VMEM(shape, BF16 if i else F32) for i, shape in enumerate(shapes)]

    past = jnp.transpose(conv_state, (0, 2, 1, 3))
    stream, kept, new = pl.pallas_call(
        functools.partial(block_kernel, nd, nt),
        out_shape=(
            pltpu.VMEM((2, half, dloc), BF16),
            pltpu.VMEM((layers, CONV_W - 1, seqs, conv_w), BF16),
            pltpu.VMEM(ssm_state.shape, F32),
        ),
        in_specs=[hbm] * 16,
        out_specs=[vmem] * 3,
        scratch_shapes=[
            pltpu.VMEM((2, half, dloc), BF16),
            pltpu.VMEM((1, seqs), jnp.int32),
            pltpu.VMEM(norm_gain.shape, F32),
            pltpu.VMEM(dt_bias.shape, F32),
            pltpu.VMEM(a_log.shape, F32),
            pltpu.VMEM(d_skip.shape, F32),
            pltpu.VMEM(out_gain.shape, F32),
            pltpu.VMEM(conv_weight.shape, BF16),
            pltpu.VMEM(past.shape, BF16),
            pltpu.VMEM(w_z.shape, BF16),
            pltpu.VMEM(w_x.shape, BF16),
            pltpu.VMEM(w_b.shape, BF16),
            pltpu.VMEM(w_c.shape, BF16),
            pltpu.VMEM(turned.shape, BF16),
            pltpu.VMEM(w_out.shape, BF16),
            *parts(2, nx),
            *parts(nd - 1)[:2],
            *parts(nx)[2:],
            *parts(max(nx - 1, 1))[2:],
            *parts(max(nx - 1, 1))[2:],
            pltpu.VMEM((layers, seqs // 8, nd, 8, width), BF16),
            *[pltpu.VMEM((layers, tiles, n, half, tile), BF16) for n in (2, nt - 1, 2)],
            *[pltpu.VMEM((batch, n), F32) for n in (heads_all, keys, width, keys, width)],
            pltpu.VMEM((seqs, conv_w), F32),
            pltpu.VMEM((width // WIDTH_X, seqs, STATE), F32),
            pltpu.VMEM((width, 128), F32),
            dma((5 + layers,)),
            dma((layers,)),
            dma((9,)),
            dma((3,)),
            dma((3,)),
            dma((3, max(nx - 1, 1))),
            dma((3, max(nx - 1, 1))),
            dma((2 + seqs // 8,)),
            dma((2 + seqs // 8,)),
            dma((2,)),
            dma((tiles,)),
            dma((1,)),
            dma((tiles, 2)),
        ],
        compiler_params=pltpu.CompilerParams(
            collective_id=0, has_side_effects=True, vmem_limit_bytes=40 * 1024 * 1024
        ),
    )(
        tokens.reshape(2, half, dloc), lengths[None, :], norm_gain, dt_bias, a_log, d_skip,
        out_gain, conv_weight, past, w_z, w_x, w_b, w_c, turned, w_out, ssm_state,
    )
    mixed_out, conv_new, ssm_new = pl.pallas_call(
        store_kernel,
        out_shape=(
            jax.ShapeDtypeStruct(stream.shape, BF16),
            jax.ShapeDtypeStruct(kept.shape, BF16),
            jax.ShapeDtypeStruct(ssm_state.shape, F32),
        ),
        in_specs=[vmem] * 3,
        out_specs=[hbm] * 3,
        scratch_shapes=[dma((3,))],
        compiler_params=pltpu.CompilerParams(vmem_limit_bytes=1024 * 1024),
    )(stream, kept, new)
    return mixed_out.reshape(batch, dloc), jnp.transpose(conv_new, (0, 2, 1, 3)), ssm_new


def solution(mesh):
    placed = (
        P("grp", "dp"),
        P(("grp", "dp")),
        P(None, "dp"),
        P(None, "dp", "tp"),
        P(None, "dp", "tp"),
        P(None, "dp", "tp"),
        P(None, "dp", "tp"),
        P(None, "dp", None),
        P(None, None, "tp"),
        P(None, "tp"),
        P(None, "tp"),
        P(None, "tp"),
        P(None, "tp"),
        P(None, "tp", "dp"),
        P(None, ("grp", "dp"), None, "tp"),
        P(None, ("grp", "dp"), "tp", None, None),
    )
    return jax.shard_map(
        functools.partial(body, mesh.shape["dp"], mesh.shape["tp"]),
        mesh=mesh,
        in_specs=placed,
        out_specs=(
            P("grp", "dp"),
            P(None, ("grp", "dp"), None, "tp"),
            P(None, ("grp", "dp"), "tp", None, None),
        ),
        check_vma=False,
    )
```
